32 devices in a mesh: grp: 2 (over x), tp: 4 (over y, core), dp: 4 (over z).
Axes of the slice: x: 2, y: 2, z: 4, core: 2. Of those that a mesh axis runs over, the one named last changes fastest.
Arguments:
- tokens: bfloat16 [512, 2048], P(('grp', 'tp'), 'dp'), parts along dimension 0, may hold values from -25 to 25
- state: float32 [2, 512, 16, 128, 128], P(None, ('grp', 'dp'), 'tp'), parts along dimension 1, may hold values from -1 to 1
- lengths: int32 [512], P(('grp', 'dp')), parts along dimension 0, may hold values from 1 to 4096, 131072 in all
- norm_gain: bfloat16 [2, 2048], P(None, 'dp'), may hold values from 0.099609375 to 1.8984375
- w_query: bfloat16 [2, 2048, 2048], P(None, 'dp', 'tp'), may hold values from -0.125 to 0.125
- w_forget: bfloat16 [2, 2048, 2048], P(None, 'dp', 'tp'), may hold values from -0.125 to 0.125
- w_input: bfloat16 [2, 2048, 2048], P(None, 'dp', 'tp'), may hold values from -0.125 to 0.125
- w_gate: bfloat16 [2, 2048, 2048], P(None, 'dp', 'tp'), may hold values from -0.125 to 0.125
- w_out: bfloat16 [2, 2048, 2048], P(None, 'tp', 'dp'), may hold values from -0.125 to 0.125
- bound_logit: float32 [2, 2048], P(None, 'tp'), may hold values from -3 to 5
- pace: float32 [2, 2048], P(None, 'tp'), may hold values from 0.6 to 2
- head_gain: float32 [2, 128], replicated, may hold values from 0.4 to 2.5
Outputs:
- mixed: float32 [512, 2048], P(('grp', 'tp'), 'dp'), parts along dimension 0
- new_state: float32 [2, 512, 16, 128, 128], P(None, ('grp', 'dp'), 'tp'), parts along dimension 1
The draws below stay inside these ranges and needn't reach their ends.
There are 2 independent parts, one for each index of `grp`. The reference program is written for one: setup_inputs(seed, part) draws one part's arguments, and reference() takes and returns one part's arrays. A program takes and returns all parts, laid end to end along the dimension named above; an argument that names none is the same for every part. Nothing has to cross between parts.
All inputs are finite; a program needn't handle non-finite values. No bound on the sum of `lengths` on one device may be relied on, other than what follows from the above.
Results may differ from the reference program's by a relative error of at most 0.0083.
Values may be sent and summed in bfloat16 or wider, within the bound.
A program may use at most 192 MiB of HBM per device.

```python
import math
import jax
import jax.numpy as jnp
import numpy as np
from jax import lax

D = 2048
HEADS = 16
HEAD = 128
KW = 2048
BATCH = 256
LENGTH_MEAN = 512
LONGEST = 4096


def draw_tokens(key, part):
    first, second = jax.random.split(jax.random.fold_in(key, 11), 2)
    level = jnp.exp(jax.random.uniform(second, (16,), jnp.float32, -1.2, 0.0))
    level = jnp.repeat(level, D // 16)
    base = jax.random.normal(first, (BATCH, D), jnp.float32)
    return jnp.clip(base * level[None, :], -25.0, 25.0).astype(jnp.bfloat16)


def draw_bound_logit(key, part):
    first, second, third = jax.random.split(jax.random.fold_in(key, 23), 3)
    quick = jax.random.bernoulli(first, 0.5, (2, HEADS))
    quick = jnp.repeat(quick, HEAD, axis=1)
    fast_values = jax.random.uniform(second, (2, KW), jnp.float32, -3.0, -1.0)
    slow_values = jax.random.uniform(third, (2, KW), jnp.float32, 2.0, 5.0)
    return jnp.where(quick, fast_values, slow_values).astype(jnp.float32)


def levels(stream_key, dims, shards, low, top_value):
    factor_of = 1.0
    for dim, blocks in shards:
        heights = jax.random.uniform(jax.random.fold_in(jax.random.fold_in(stream_key, 6), dim), (blocks,), jnp.float32, low / len(shards), top_value / len(shards))
        factor_of = factor_of * jnp.repeat(jnp.exp(heights), dims[dim] // blocks).reshape((-1,) + (1,) * (len(dims) - 1 - dim))
    return factor_of


def length_profile(amount, total, bound, lean):
    weights = [(1 << 20) // math.isqrt(standing ** lean) + 1 for standing in range(2, amount + 1)]
    rest, holding = total - bound - (amount - 1), [1] * (amount - 1)
    while rest > 0:
        candidates = [i for i in range(amount - 1) if holding[i] < bound]
        pool, remaining = sum([weights[i] for i in candidates]), rest
        for i in candidates:
            more = min(bound - holding[i], max(1, remaining * weights[i] // pool), rest)
            holding[i] = holding[i] + more
            rest = rest - more
    return np.array([bound] + holding)


def ragged_sizes(rng, amount, total, bound, skew):
    if amount == 2:
        one = jax.random.randint(rng, (), max(1, total - bound), min(bound, total - 1) + 1)
        return jnp.stack([one, total - one])
    sizes = jnp.asarray(length_profile(amount, total, bound, skew), jnp.int32)
    pairs = (amount - 1) // 2
    giver, taker = sizes[1:1 + 2 * pairs:2], sizes[2:2 + 2 * pairs:2]
    slack = jnp.minimum(giver - 1, bound - taker)
    shifted = jax.random.randint(jax.random.fold_in(rng, 1), (pairs,), 0, 1 << 20) % (slack + 1)
    sizes = sizes.at[1:1 + 2 * pairs:2].set(giver - shifted).at[2:2 + 2 * pairs:2].set(taker + shifted)
    return sizes[jax.random.permutation(jax.random.fold_in(rng, 2), amount)]


def noise(own_key, shape, deviation, most, cuts=(), kind=jnp.bfloat16):
    loudness = levels(own_key, shape, cuts, -0.22, 0.18) if cuts else 1.0
    entries = jax.random.normal(own_key, shape, jnp.float32) * deviation * loudness
    return jnp.minimum(jnp.maximum(entries, -most), most).astype(kind)


def setup_inputs(seed: int = 0, part: int = 0) -> dict:
    streams_of = jax.random.split(jax.random.key(seed), 13)
    own_keys = jax.random.split(jax.random.fold_in(streams_of[12], part), 13)
    tokens = draw_tokens(jax.random.fold_in(jax.random.fold_in(streams_of[12], part), 71), part)
    state = noise(own_keys[1], (2, BATCH, HEADS, HEAD, HEAD), 0.15, 1.0, ((1, 4), (2, 4)), jnp.float32)
    lengths = ragged_sizes(own_keys[2], BATCH, BATCH * LENGTH_MEAN, LONGEST, 2).astype(jnp.int32)
    norm_gain = jnp.clip(1.0 + 0.18 * jax.random.normal(streams_of[3], (2, D), jnp.float32), 0.099609375, 1.8984375).astype(jnp.bfloat16)
    w_query = noise(streams_of[4], (2, D, KW), D ** -0.5, 0.125, ((1, 4), (2, 4)))
    w_forget = noise(streams_of[5], (2, D, KW), D ** -0.5, 0.125, ((1, 4), (2, 4)))
    w_input = noise(streams_of[6], (2, D, KW), D ** -0.5, 0.125, ((1, 4), (2, 4)))
    w_gate = noise(streams_of[7], (2, D, KW), D ** -0.5, 0.125, ((1, 4), (2, 4)))
    w_out = noise(streams_of[8], (2, KW, D), KW ** -0.5, 0.125, ((1, 4), (2, 4)))
    bound_logit = draw_bound_logit(jax.random.fold_in(streams_of[12], 71), part)
    pace = jnp.clip(jnp.exp(math.log(2.0) - 1.2039728 * jax.random.uniform(streams_of[10], (2, KW), jnp.float32) ** levels(streams_of[10], (2, KW), ((1, 4),), -0.2, 0.2)), 0.6, 2.0)
    head_gain = jnp.clip(jnp.exp(jax.random.uniform(streams_of[11], (2, HEAD), jnp.float32, math.log(0.4), math.log(2.5))), 0.4, 2.5)
    return {"tokens": tokens, "state": state, "lengths": lengths, "norm_gain": norm_gain, "w_query": w_query, "w_forget": w_forget, "w_input": w_input, "w_gate": w_gate, "w_out": w_out, "bound_logit": bound_logit, "pace": pace, "head_gain": head_gain}


epsilon = 1e-06

def advance(prior, query, forget_in, value, gate, lower, pace_row, log_len, gain_row):
    count, width = query.shape
    size = prior.shape[-1]
    heads = width // size
    pre = forget_in - pace_row[None, :] * log_len[:, None]
    forget = lower[None, :] + (1.0 - lower[None, :]) * jax.nn.sigmoid(pre)
    key = (1.0 - lower[None, :]) * jax.nn.sigmoid(-pre)
    forget = forget.reshape(count, heads, size)
    key = key.reshape(count, heads, size)
    values = value.reshape(count, heads, size)
    updated = forget[..., None] * prior + key[..., None] * values[:, :, None, :]
    readout = jnp.einsum('bhk,bhkv->bhv', query.reshape(count, heads, size), updated, precision=lax.Precision.HIGHEST)
    normed = readout * lax.rsqrt(lax.optimization_barrier(jnp.mean(readout * readout, axis=-1, keepdims=True)) + epsilon)
    gates = gate.reshape(count, heads, size)
    normed = normed * gain_row[None, None, :] * jax.nn.silu(gates)
    return (updated, normed.reshape(count, width).astype(jnp.bfloat16))

def reference(tokens, state, lengths, norm_gain, w_query, w_forget, w_input, w_gate, w_out, bound_logit, pace, head_gain):
    current = tokens
    log_len = jnp.log(lengths.astype(jnp.float32) / LENGTH_MEAN)
    states = []
    result = None
    for block in range(2):
        wide = current.astype(jnp.float32)
        squares = lax.optimization_barrier(jnp.sum(wide * wide, axis=1))
        scale = lax.rsqrt(squares / D + epsilon)
        gained = (wide * norm_gain[block].astype(jnp.float32)[None, :]).astype(jnp.bfloat16)
        made = []
        for weight in (w_query[block], w_forget[block], w_input[block], w_gate[block]):
            made.append(scale[:, None] * jnp.dot(gained, weight, preferred_element_type=jnp.float32))
        lower = jax.nn.sigmoid(bound_logit[block])
        updated, normed = advance(state[block], made[0], made[1], made[2], made[3], lower, pace[block], log_len, head_gain[block])
        states.append(updated)
        branch = jnp.dot(normed, w_out[block], preferred_element_type=jnp.float32)
        if block == 0:
            current = (wide + branch).astype(jnp.bfloat16)
        else:
            result = wide + branch
    return (result, jnp.stack(states))
```

```python
import functools

import jax
import jax.numpy as jnp
from jax import lax
from jax.experimental import pallas as pl
from jax.experimental.pallas import tpu as pltpu
from jax.sharding import PartitionSpec as P

LENGTH_MEAN = 512
epsilon = 1e-06
GROUP = 8
MESH_ID = pl.DeviceIdType.MESH
f32 = jnp.float32
bf16 = jnp.bfloat16


def chain(
    n_tp,
    n_dp,
    width,
    tokens,
    state,
    lengths,
    gain,
    w_query,
    w_forget,
    w_input,
    w_gate,
    w_out,
    bound,
    pace,
    head_gain,
    mixed,
    forget_o,
    key_o,
    value_o,
    xall,
    sbuf,
    wbuf,
    wobuf,
    psend,
    precv,
    pown,
    nall,
    osend,
    orecv,
    oown,
    gate_s,
    qf_s,
    qk_s,
    ro_s,
    w_sem,
    s_sem,
    x_ss,
    x_rs,
    p_ss,
    p_rs,
    n_ss,
    n_rs,
    o_ss,
    o_rs,
):
    t, d = lax.axis_index("tp"), lax.axis_index("dp")
    rt, feats = tokens.shape
    own, heads, size = state.shape[1], state.shape[2], state.shape[3]
    chans = heads * size
    groups = own // GROUP

    def tp_peer(k):
        return lax.rem(t + k, n_tp)

    def dp_peer(k):
        return lax.rem(d + k, n_dp)

    loads = []
    for b in range(2):
        per = []
        for i, w in enumerate((w_query, w_forget, w_input, w_gate)):
            per.append(pltpu.make_async_copy(w.at[b], wbuf.at[b, i], w_sem.at[b, i]))
        per.append(pltpu.make_async_copy(w_out.at[b], wobuf.at[b], w_sem.at[b, 4]))
        loads.append(per)

    def state_load(b, g):
        rows = pl.ds(g * GROUP, GROUP)
        return pltpu.make_async_copy(state.at[b, rows], sbuf.at[b, rows], s_sem.at[b, g])

    for c in loads[0]:
        c.start()

    barrier = pltpu.get_barrier_semaphore()
    for k in range(1, n_tp):
        pl.semaphore_signal(barrier, inc=1, device_id={"tp": tp_peer(k)}, device_id_type=MESH_ID)
    for k in range(1, n_dp):
        pl.semaphore_signal(barrier, inc=1, device_id={"dp": dp_peer(k)}, device_id_type=MESH_ID)
    pl.semaphore_wait(barrier, n_tp + n_dp - 2)

    my_rows = pl.ds(pl.multiple_of(t * rt, rt), rt)
    my_seqs = pl.ds(pl.multiple_of(d * own, own), own)
    sends = []
    current = tokens[...].astype(f32)
    log_len = jnp.log(lengths[...].astype(f32) / LENGTH_MEAN)
    lane = lax.broadcasted_iota(jnp.int32, (own, 128), 1)
    row_id = lax.broadcasted_iota(jnp.int32, (GROUP, size), 0)

    for b in range(2):
        copies = []
        for k in range(1, n_tp):
            c = pltpu.make_async_remote_copy(
                src_ref=tokens if b == 0 else xall.at[b, my_rows],
                dst_ref=xall.at[b, my_rows],
                send_sem=x_ss.at[b, k - 1],
                recv_sem=x_rs.at[b, k - 1],
                device_id={"tp": tp_peer(k)},
                device_id_type=MESH_ID,
            )
            c.start()
            copies.append(c)
        sends += copies
        if b == 0:
            xall[b, my_rows, :] = tokens[...]
            for g in range(groups):
                state_load(0, g).start()
            for c in loads[1]:
                c.start()
            for g in range(groups):
                state_load(1, g).start()
        for i in range(4):
            loads[b][i].wait()
        for c in copies:
            c.wait_recv()

        gain_row = gain[b : b + 1, :].astype(f32)
        copies = []
        for k in [n_dp // 2] + [k for k in range(1, n_dp) if k != n_dp // 2] + [0]:
            dest = dp_peer(k)
            x = xall[b, pl.ds(pl.multiple_of(dest * own, own), own), :].astype(f32)
            sq = jnp.sum(x * x, axis=1, keepdims=True)
            gained = (x * gain_row).astype(bf16)
            for i in range(4):
                part = jnp.dot(gained, wbuf[b, i], preferred_element_type=f32)
                if k == 0:
                    pown[:, i * chans : (i + 1) * chans] = part
                else:
                    psend[b, k - 1, :, i * chans : (i + 1) * chans] = part.astype(bf16)
            if k == 0:
                own_sq = sq
            else:
                hi = sq.astype(bf16).astype(f32)
                packed = jnp.where(lane == 0, hi, jnp.where(lane == 1, sq - hi, 0.0))
                psend[b, k - 1, :, 4 * chans :] = packed.astype(bf16)
                c = pltpu.make_async_remote_copy(
                    src_ref=psend.at[b, k - 1],
                    dst_ref=precv.at[b, k - 1],
                    send_sem=p_ss.at[b, k - 1],
                    recv_sem=p_rs.at[b, k - 1],
                    device_id={"dp": dest},
                    device_id_type=MESH_ID,
                )
                c.start()
                copies.append(c)
        sends += copies
        for c in copies:
            c.wait_recv()

        squares = own_sq
        for k in range(n_dp - 1):
            squares = squares + jnp.sum(precv[b, k, :, 4 * chans :].astype(f32), axis=1, keepdims=True)
        scale = lax.rsqrt(squares / width + epsilon)

        def total(i):
            cols = slice(i * chans, (i + 1) * chans)
            acc = pown[:, cols]
            for k in range(n_dp - 1):
                acc = acc + precv[b, k, :, cols].astype(f32)
            return scale * acc

        lower = jax.nn.sigmoid(bound[b : b + 1, :])
        pre = total(1) - pace[b : b + 1, :] * log_len
        forget = lower + (1.0 - lower) * jax.nn.sigmoid(pre)
        key = (1.0 - lower) * jax.nn.sigmoid(-pre)
        forget_o[b] = forget
        key_o[b] = key
        query = total(0)
        qf_s[...] = query * forget
        qk_s[...] = query * key
        value_o[b] = total(2)
        gate = total(3)
        gate_s[...] = gate * jax.nn.sigmoid(gate)

        for g in range(groups):
            state_load(b, g).wait()

        def read(g, carry):
            rows = pl.ds(pl.multiple_of(g * GROUP, GROUP), GROUP)
            for h in range(heads):
                cols = slice(h * size, (h + 1) * size)
                q8 = qf_s[rows, cols]
                diag = jnp.concatenate(
                    [jnp.where(row_id == j, q8, 0.0) for j in range(GROUP)], axis=1
                ).astype(bf16)
                s8 = sbuf[b, rows, h].reshape(GROUP * size, size).astype(bf16)
                ro_s[rows, cols] = jnp.dot(diag, s8, preferred_element_type=f32)
            return carry

        lax.fori_loop(0, groups, read, 0)
        for h in range(heads):
            cols = slice(h * size, (h + 1) * size)
            dots = jnp.sum(qk_s[:, cols], axis=1, keepdims=True)
            readout = ro_s[:, cols] + dots * value_o[b, :, cols]
            mean = jnp.mean(readout * readout, axis=1, keepdims=True)
            normed = readout * lax.rsqrt(mean + epsilon) * head_gain[b : b + 1, :] * gate_s[:, cols]
            nall[b, my_seqs, cols] = normed.astype(bf16)

        copies = []
        for k in range(1, n_dp):
            c = pltpu.make_async_remote_copy(
                src_ref=nall.at[b, my_seqs],
                dst_ref=nall.at[b, my_seqs],
                send_sem=n_ss.at[b, k - 1],
                recv_sem=n_rs.at[b, k - 1],
                device_id={"dp": dp_peer(k)},
                device_id_type=MESH_ID,
            )
            c.start()
            copies.append(c)
        sends += copies
        loads[b][4].wait()
        for c in copies:
            c.wait_recv()

        copies = []
        for k in list(range(1, n_tp)) + [0]:
            dest = tp_peer(k)
            rows = nall[b, pl.ds(pl.multiple_of(dest * rt, rt), rt), :]
            part = jnp.dot(rows, wobuf[b], preferred_element_type=f32)
            if k == 0:
                oown[...] = part
            else:
                osend[b, k - 1] = part.astype(bf16)
                c = pltpu.make_async_remote_copy(
                    src_ref=osend.at[b, k - 1],
                    dst_ref=orecv.at[b, k - 1],
                    send_sem=o_ss.at[b, k - 1],
                    recv_sem=o_rs.at[b, k - 1],
                    device_id={"tp": dest},
                    device_id_type=MESH_ID,
                )
                c.start()
                copies.append(c)
        sends += copies
        for c in copies:
            c.wait_recv()
        branch = oown[...]
        for k in range(n_tp - 1):
            branch = branch + orecv[b, k].astype(f32)
        if b == 0:
            rounded = (current + branch).astype(bf16)
            xall[1, my_rows, :] = rounded
            current = rounded.astype(f32)
        else:
            mixed[...] = current + branch

    for c in sends:
        c.wait_send()


def update(state, forget, key, value, out):
    heads, size = state.shape[2], state.shape[3]
    for h in range(heads):
        cols = slice(h * size, (h + 1) * size)
        f_t = forget[0, :, cols].T
        k_t = key[0, :, cols].T
        v = value[0, :, cols]
        for j in range(GROUP):
            out[0, j, h] = f_t[:, j : j + 1] * state[0, j, h] + k_t[:, j : j + 1] * v[j : j + 1, :]


def shards(n_tp, n_dp, tokens, state, lengths, gain, w_query, w_forget, w_input, w_gate, w_out, bound, pace, head_gain):
    rt, feats = tokens.shape
    own, heads, size = state.shape[1:4]
    chans = heads * size
    rows = rt * n_tp
    msg = 4 * chans + 128
    vmem = pl.BlockSpec(memory_space=pltpu.VMEM)
    hbm = pl.BlockSpec(memory_space=pl.ANY)
    gates = jax.ShapeDtypeStruct((2, own, chans), f32)
    dma = pltpu.SemaphoreType.DMA
    mixed, forget, key, value = pl.pallas_call(
        functools.partial(chain, n_tp, n_dp, feats * n_dp),
        name="chain",
        out_shape=(jax.ShapeDtypeStruct((rt, feats), f32), gates, gates, gates),
        in_specs=[vmem, hbm, vmem, vmem] + [hbm] * 5 + [vmem] * 3,
        out_specs=(vmem,) * 4,
        scratch_shapes=[
            pltpu.VMEM((2, rows, feats), bf16),
            pltpu.VMEM((2, own, heads, size, size), f32),
            pltpu.VMEM((2, 4, feats, chans), bf16),
            pltpu.VMEM((2, chans, feats), bf16),
            pltpu.VMEM((2, n_dp - 1, own, msg), bf16),
            pltpu.VMEM((2, n_dp - 1, own, msg), bf16),
            pltpu.VMEM((own, 4 * chans), f32),
            pltpu.VMEM((2, rows, chans), bf16),
            pltpu.VMEM((2, n_tp - 1, rt, feats), bf16),
            pltpu.VMEM((2, n_tp - 1, rt, feats), bf16),
            pltpu.VMEM((rt, feats), f32),
            pltpu.VMEM((own, chans), f32),
            pltpu.VMEM((own, chans), f32),
            pltpu.VMEM((own, chans), f32),
            pltpu.VMEM((own, chans), f32),
            dma((2, 5)),
            dma((2, own // GROUP)),
            dma((2, n_tp - 1)),
            dma((2, n_tp - 1)),
            dma((2, n_dp - 1)),
            dma((2, n_dp - 1)),
            dma((2, n_dp - 1)),
            dma((2, n_dp - 1)),
            dma((2, n_tp - 1)),
            dma((2, n_tp - 1)),
        ],
        compiler_params=pltpu.CompilerParams(
            collective_id=0, has_side_effects=True, vmem_limit_bytes=60 * 1024 * 1024
        ),
    )(tokens, state, lengths[:, None], gain, w_query, w_forget, w_input, w_gate, w_out, bound, pace, head_gain)

    block = pl.BlockSpec((1, GROUP, heads, size, size), lambda b, g: (b, g, 0, 0, 0))
    row = pl.BlockSpec((1, GROUP, chans), lambda b, g: (b, g, 0))
    new_state = pl.pallas_call(
        update,
        name="update",
        grid=(2, own // GROUP),
        out_shape=jax.ShapeDtypeStruct(state.shape, f32),
        in_specs=[block, row, row, row],
        out_specs=block,
    )(state, forget, key, value)
    return mixed, new_state


def solution(mesh):
    in_specs = (
        P(("grp", "tp"), "dp"),
        P(None, ("grp", "dp"), "tp", None, None),
        P(("grp", "dp")),
        P(None, "dp"),
        P(None, "dp", "tp"),
        P(None, "dp", "tp"),
        P(None, "dp", "tp"),
        P(None, "dp", "tp"),
        P(None, "tp", "dp"),
        P(None, "tp"),
        P(None, "tp"),
        P(),
    )
    out_specs = (P(("grp", "tp"), "dp"), P(None, ("grp", "dp"), "tp", None, None))
    body = functools.partial(shards, mesh.shape["tp"], mesh.shape["dp"])
    return jax.shard_map(body, mesh=mesh, in_specs=in_specs, out_specs=out_specs, check_vma=False)
```

```python
import functools

import jax
import jax.numpy as jnp
from jax import lax
from jax.experimental import pallas as pl
from jax.experimental.pallas import tpu as pltpu
from jax.sharding import PartitionSpec as P

LENGTH_MEAN = 512
epsilon = 1e-06
GROUP = 8
LIMIT = 26 * 1024 * 1024
MESH_ID = pl.DeviceIdType.MESH
f32 = jnp.float32
bf16 = jnp.bfloat16


def chain(
    n_tp,
    n_dp,
    width,
    tokens,
    state,
    lengths,
    gain,
    w_query,
    w_forget,
    w_input,
    w_gate,
    w_out,
    bound,
    pace,
    head_gain,
    mixed,
    sbuf,
    forget_o,
    key_o,
    value_o,
    xall,
    wbuf,
    wobuf,
    psend,
    precv,
    pown,
    nall,
    osend,
    orecv,
    oown,
    gate_s,
    qf_s,
    qk_s,
    ro_s,
    w_sem,
    s_sem,
    x_ss,
    x_rs,
    p_ss,
    p_rs,
    n_ss,
    n_rs,
    o_ss,
    o_rs,
):
    t, d = lax.axis_index("tp"), lax.axis_index("dp")
    rt, feats = tokens.shape
    own, heads, size = state.shape[1], state.shape[2], state.shape[3]
    chans = heads * size
    groups = own // GROUP

    def tp_peer(k):
        return lax.rem(t + k, n_tp)

    def dp_peer(k):
        return lax.rem(d + k, n_dp)

    loads = []
    for b in range(2):
        per = []
        for i, w in enumerate((w_query, w_forget, w_input, w_gate)):
            per.append(pltpu.make_async_copy(w.at[b], wbuf.at[b, i], w_sem.at[b, i]))
        per.append(pltpu.make_async_copy(w_out.at[b], wobuf.at[b], w_sem.at[b, 4]))
        loads.append(per)

    def state_load(b, g):
        rows = pl.ds(g * GROUP, GROUP)
        return pltpu.make_async_copy(state.at[b, rows], sbuf.at[b, rows], s_sem.at[b, g])

    for c in loads[0]:
        c.start()

    barrier = pltpu.get_barrier_semaphore()
    for k in range(1, n_tp):
        pl.semaphore_signal(barrier, inc=1, device_id={"tp": tp_peer(k)}, device_id_type=MESH_ID)
    for k in range(1, n_dp):
        pl.semaphore_signal(barrier, inc=1, device_id={"dp": dp_peer(k)}, device_id_type=MESH_ID)
    pl.semaphore_wait(barrier, n_tp + n_dp - 2)

    my_rows = pl.ds(pl.multiple_of(t * rt, rt), rt)
    my_seqs = pl.ds(pl.multiple_of(d * own, own), own)
    sends = []
    current = tokens[...].astype(f32)
    log_len = jnp.log(lengths[...].astype(f32) / LENGTH_MEAN)
    lane = lax.broadcasted_iota(jnp.int32, (own, 128), 1)
    row_id = lax.broadcasted_iota(jnp.int32, (GROUP, size), 0)

    def advance(b, g, carry):
        rows = pl.ds(pl.multiple_of(g * GROUP, GROUP), GROUP)
        for h in range(heads):
            cols = slice(h * size, (h + 1) * size)
            f_t = forget_o[b, rows, cols].T
            k_t = key_o[b, rows, cols].T
            v = value_o[b, rows, cols]
            for j in range(GROUP):
                at = g * GROUP + j
                sbuf[b, at, h] = f_t[:, j : j + 1] * sbuf[b, at, h] + k_t[:, j : j + 1] * v[j : j + 1, :]
        return carry

    for b in range(2):
        copies = []
        for k in range(1, n_tp):
            c = pltpu.make_async_remote_copy(
                src_ref=tokens if b == 0 else xall.at[b, my_rows],
                dst_ref=xall.at[b, my_rows],
                send_sem=x_ss.at[b, k - 1],
                recv_sem=x_rs.at[b, k - 1],
                device_id={"tp": tp_peer(k)},
                device_id_type=MESH_ID,
            )
            c.start()
            copies.append(c)
        sends += copies
        if b == 0:
            xall[b, my_rows, :] = tokens[...]
            for g in range(groups):
                state_load(0, g).start()
            for c in loads[1]:
                c.start()
            for g in range(groups):
                state_load(1, g).start()
        for i in range(4):
            loads[b][i].wait()
        for c in copies:
            c.wait_recv()

        gain_row = gain[b : b + 1, :].astype(f32)
        copies = []
        for k in [n_dp // 2] + [k for k in range(1, n_dp) if k != n_dp // 2] + [0]:
            dest = dp_peer(k)
            x = xall[b, pl.ds(pl.multiple_of(dest * own, own), own), :].astype(f32)
            sq = jnp.sum(x * x, axis=1, keepdims=True)
            gained = (x * gain_row).astype(bf16)
            for i in range(4):
                part = jnp.dot(gained, wbuf[b, i], preferred_element_type=f32)
                if k == 0:
                    pown[:, i * chans : (i + 1) * chans] = part
                else:
                    psend[b, k - 1, :, i * chans : (i + 1) * chans] = part.astype(bf16)
            if k == 0:
                own_sq = sq
            else:
                hi = sq.astype(bf16).astype(f32)
                packed = jnp.where(lane == 0, hi, jnp.where(lane == 1, sq - hi, 0.0))
                psend[b, k - 1, :, 4 * chans :] = packed.astype(bf16)
                c = pltpu.make_async_remote_copy(
                    src_ref=psend.at[b, k - 1],
                    dst_ref=precv.at[b, k - 1],
                    send_sem=p_ss.at[b, k - 1],
                    recv_sem=p_rs.at[b, k - 1],
                    device_id={"dp": dest},
                    device_id_type=MESH_ID,
                )
                c.start()
                copies.append(c)
        sends += copies
        if b == 1:
            lax.fori_loop(0, groups, functools.partial(advance, 0), 0)
        for c in copies:
            c.wait_recv()

        squares = own_sq
        for k in range(n_dp - 1):
            squares = squares + jnp.sum(precv[b, k, :, 4 * chans :].astype(f32), axis=1, keepdims=True)
        scale = lax.rsqrt(squares / width + epsilon)

        def total(i):
            cols = slice(i * chans, (i + 1) * chans)
            acc = pown[:, cols]
            for k in range(n_dp - 1):
                acc = acc + precv[b, k, :, cols].astype(f32)
            return scale * acc

        lower = jax.nn.sigmoid(bound[b : b + 1, :])
        pre = total(1) - pace[b : b + 1, :] * log_len
        forget = lower + (1.0 - lower) * jax.nn.sigmoid(pre)
        key = (1.0 - lower) * jax.nn.sigmoid(-pre)
        forget_o[b] = forget
        key_o[b] = key
        query = total(0)
        qf_s[...] = query * forget
        qk_s[...] = query * key
        value_o[b] = total(2)
        gate = total(3)
        gate_s[...] = gate * jax.nn.sigmoid(gate)

        for g in range(groups):
            state_load(b, g).wait()

        def read(g, carry):
            rows = pl.ds(pl.multiple_of(g * GROUP, GROUP), GROUP)
            for h in range(heads):
                cols = slice(h * size, (h + 1) * size)
                q8 = qf_s[rows, cols]
                diag = jnp.concatenate(
                    [jnp.where(row_id == j, q8, 0.0) for j in range(GROUP)], axis=1
                ).astype(bf16)
                s8 = sbuf[b, rows, h].reshape(GROUP * size, size).astype(bf16)
                ro_s[rows, cols] = jnp.dot(diag, s8, preferred_element_type=f32)
            return carry

        lax.fori_loop(0, groups, read, 0)
        for h in range(heads):
            cols = slice(h * size, (h + 1) * size)
            dots = jnp.sum(qk_s[:, cols], axis=1, keepdims=True)
            readout = ro_s[:, cols] + dots * value_o[b, :, cols]
            mean = jnp.mean(readout * readout, axis=1, keepdims=True)
            normed = readout * lax.rsqrt(mean + epsilon) * head_gain[b : b + 1, :] * gate_s[:, cols]
            nall[b, my_seqs, cols] = normed.astype(bf16)

        copies = []
        for k in range(1, n_dp):
            c = pltpu.make_async_remote_copy(
                src_ref=nall.at[b, my_seqs],
                dst_ref=nall.at[b, my_seqs],
                send_sem=n_ss.at[b, k - 1],
                recv_sem=n_rs.at[b, k - 1],
                device_id={"dp": dp_peer(k)},
                device_id_type=MESH_ID,
            )
            c.start()
            copies.append(c)
        sends += copies
        loads[b][4].wait()
        if b == 1:
            lax.fori_loop(0, groups, functools.partial(advance, 1), 0)
        for c in copies:
            c.wait_recv()

        copies = []
        for k in list(range(1, n_tp)) + [0]:
            dest = tp_peer(k)
            rows = nall[b, pl.ds(pl.multiple_of(dest * rt, rt), rt), :]
            part = jnp.dot(rows, wobuf[b], preferred_element_type=f32)
            if k == 0:
                oown[...] = part
            else:
                osend[b, k - 1] = part.astype(bf16)
                c = pltpu.make_async_remote_copy(
                    src_ref=osend.at[b, k - 1],
                    dst_ref=orecv.at[b, k - 1],
                    send_sem=o_ss.at[b, k - 1],
                    recv_sem=o_rs.at[b, k - 1],
                    device_id={"tp": dest},
                    device_id_type=MESH_ID,
                )
                c.start()
                copies.append(c)
        sends += copies
        for c in copies:
            c.wait_recv()
        branch = oown[...]
        for k in range(n_tp - 1):
            branch = branch + orecv[b, k].astype(f32)
        if b == 0:
            rounded = (current + branch).astype(bf16)
            xall[1, my_rows, :] = rounded
            current = rounded.astype(f32)
        else:
            mixed[...] = current + branch

    for c in sends:
        c.wait_send()


def store(mixed, new_state, mixed_out, state_out, sems):
    blocks, own = new_state.shape[:2]
    copies = [pltpu.make_async_copy(mixed, mixed_out, sems.at[blocks, 0])]
    for b in range(blocks):
        for g in range(own // GROUP):
            rows = pl.ds(g * GROUP, GROUP)
            copies.append(pltpu.make_async_copy(new_state.at[b, rows], state_out.at[b, rows], sems.at[b, g]))
    for c in copies:
        c.start()
    for c in copies:
        c.wait()


def shards(n_tp, n_dp, tokens, state, lengths, gain, w_query, w_forget, w_input, w_gate, w_out, bound, pace, head_gain):
    rt, feats = tokens.shape
    own, heads, size = state.shape[1:4]
    chans = heads * size
    rows = rt * n_tp
    msg = 4 * chans + 128
    vmem = pl.BlockSpec(memory_space=pltpu.VMEM)
    hbm = pl.BlockSpec(memory_space=pl.ANY)
    gates = pltpu.VMEM((2, own, chans), f32)
    dma = pltpu.SemaphoreType.DMA
    mixed, new_state = pl.pallas_call(
        functools.partial(chain, n_tp, n_dp, feats * n_dp),
        name="chain",
        out_shape=(pltpu.VMEM((rt, feats), f32), pltpu.VMEM(state.shape, f32)),
        in_specs=[vmem, hbm, vmem, vmem] + [hbm] * 5 + [vmem] * 3,
        out_specs=(vmem, vmem),
        scratch_shapes=[
            gates,
            gates,
            gates,
            pltpu.VMEM((2, rows, feats), bf16),
            pltpu.VMEM((2, 4, feats, chans), bf16),
            pltpu.VMEM((2, chans, feats), bf16),
            pltpu.VMEM((2, n_dp - 1, own, msg), bf16),
            pltpu.VMEM((2, n_dp - 1, own, msg), bf16),
            pltpu.VMEM((own, 4 * chans), f32),
            pltpu.VMEM((2, rows, chans), bf16),
            pltpu.VMEM((2, n_tp - 1, rt, feats), bf16),
            pltpu.VMEM((2, n_tp - 1, rt, feats), bf16),
            pltpu.VMEM((rt, feats), f32),
            pltpu.VMEM((own, chans), f32),
            pltpu.VMEM((own, chans), f32),
            pltpu.VMEM((own, chans), f32),
            pltpu.VMEM((own, chans), f32),
            dma((2, 5)),
            dma((2, own // GROUP)),
            dma((2, n_tp - 1)),
            dma((2, n_tp - 1)),
            dma((2, n_dp - 1)),
            dma((2, n_dp - 1)),
            dma((2, n_dp - 1)),
            dma((2, n_dp - 1)),
            dma((2, n_tp - 1)),
            dma((2, n_tp - 1)),
        ],
        compiler_params=pltpu.CompilerParams(
            collective_id=0, has_side_effects=True, vmem_limit_bytes=LIMIT
        ),
    )(tokens, state, lengths[:, None], gain, w_query, w_forget, w_input, w_gate, w_out, bound, pace, head_gain)

    return pl.pallas_call(
        store,
        name="store",
        out_shape=(jax.ShapeDtypeStruct((rt, feats), f32), jax.ShapeDtypeStruct(state.shape, f32)),
        in_specs=[vmem, vmem],
        out_specs=(hbm, hbm),
        scratch_shapes=[dma((3, own // GROUP))],
        compiler_params=pltpu.CompilerParams(vmem_limit_bytes=LIMIT),
    )(pltpu.with_memory_space_constraint(mixed, pltpu.VMEM), pltpu.with_memory_space_constraint(new_state, pltpu.VMEM))


def solution(mesh):
    in_specs = (
        P(("grp", "tp"), "dp"),
        P(None, ("grp", "dp"), "tp", None, None),
        P(("grp", "dp")),
        P(None, "dp"),
        P(None, "dp", "tp"),
        P(None, "dp", "tp"),
        P(None, "dp", "tp"),
        P(None, "dp", "tp"),
        P(None, "tp", "dp"),
        P(None, "tp"),
        P(None, "tp"),
        P(),
    )
    out_specs = (P(("grp", "tp"), "dp"), P(None, ("grp", "dp"), "tp", None, None))
    body = functools.partial(shards, mesh.shape["tp"], mesh.shape["dp"])
    return jax.shard_map(body, mesh=mesh, in_specs=in_specs, out_specs=out_specs, check_vma=False)
```
